512 devices in a mesh: grp: 2 (over y), sp: 64 (over z, core), tp: 4 (over x).
Axes of the slice: x: 4, y: 2, z: 32, core: 2. Of those that a mesh axis runs over, the one named last changes fastest.
The devices are a block of a 4x8x32 slice.
Arguments:
- tokens: bfloat16 [16384, 2048], P(('grp', 'sp'), 'tp'), parts along dimension 0, may hold values from -6 to 6
- norm_gain: float32 [2048], replicated, may hold values from 0.1 to 1.9
- att_q_weight: bfloat16 [1024, 2048], P('tp', 'sp'), may hold values from -0.625 to 0.625
- att_k_weight: bfloat16 [512, 2048], P('tp', 'sp'), may hold values from -0.125 to 0.125
- att_v_weight: bfloat16 [512, 2048], P('tp', 'sp'), may hold values from -0.125 to 0.125
- rec_q_weight: bfloat16 [1024, 2048], P('tp', 'sp'), may hold values from -0.125 to 0.125
- rec_f_weight: bfloat16 [1024, 2048], P('tp', 'sp'), may hold values from -0.125 to 0.125
- rec_i_weight: bfloat16 [1024, 2048], P('tp', 'sp'), may hold values from -0.125 to 0.125
- att_out_weight: bfloat16 [1024, 2048], P('tp', 'sp'), may hold values from -1.5 to 1.5
- rec_out_weight: bfloat16 [1024, 2048], P('tp', 'sp'), may hold values from -0.1875 to 0.1875
- score_offset: float32 [16], P('tp'), may hold values from -11.5 to -3
- lower_bound: float32 [1024], P('tp'), may hold values from 0.94 to 0.99999
- decay_shift: float32 [16384, 1024], P(('grp', 'sp'), 'tp'), parts along dimension 0, may hold values from -2.1 to 0
- rec_gain: float32 [1024], P('tp'), may hold values from 0.1 to 1.9
Outputs:
- mixed: bfloat16 [16384, 2048], P(('grp', 'sp', 'tp')), parts along dimension 0
The draws below stay inside these ranges and needn't reach their ends.
There are 2 independent parts, one for each index of `grp`. The reference program is written for one: setup_inputs(seed, part) draws one part's arguments, and reference() takes and returns one part's arrays. A program takes and returns all parts, laid end to end along the dimension named above; an argument that names none is the same for every part. Nothing has to cross between parts.
All inputs are finite; a program needn't handle non-finite values.
Results may differ from the reference program's by a relative error of at most 0.015.
Values may be sent and summed in bfloat16 or wider, within the bound.
A program may use at most 64 MiB of HBM per device.

```python
import math
import jax
import jax.numpy as jnp
from jax import lax

D = 2048
ATT_HEADS = 16
KV_HEADS = 8
HEAD = 64
RECURRENT_COUNT = 8
REC_KEY = 128
REC_VAL = 128
SPAN = 64
TOK_DEV = 128
SEQ = 8192
ATT_WIDTH = 1024
KV_WIDTH = 512
KEY_WIDTH = 1024
VAL_WIDTH = 1024
N_TP = 4


def draw_score_offset(key, part):
    order = jax.random.permutation(jax.random.fold_in(key, 11), ATT_HEADS)
    level = jax.random.uniform(jax.random.fold_in(key, 12), (ATT_HEADS,), jnp.float32)
    slow = order >= ATT_HEADS // 2
    far = -11.5 + 1.5 * level
    near = -6.0 + 3.0 * level
    return jnp.where(slow, far, near).astype(jnp.float32)


def draw_lower_bound(key, part):
    order = jax.random.permutation(jax.random.fold_in(key, 21), RECURRENT_COUNT)
    slow = order >= RECURRENT_COUNT // 2
    level = jax.random.uniform(jax.random.fold_in(key, 22), (RECURRENT_COUNT, REC_KEY), jnp.float32)
    slow_gap = jnp.exp(math.log(1.5e-05) + level * math.log(5e-05 / 1.5e-05))
    fast_gap = jnp.exp(math.log(0.02) + level * math.log(3.0))
    gap = jnp.where(slow[:, None], slow_gap, fast_gap)
    return (1.0 - gap).reshape(KEY_WIDTH).astype(jnp.float32)


def draw_decay_shift(key, part):
    blocks = SEQ // TOK_DEV
    level = jax.random.uniform(jax.random.fold_in(key, 31), (blocks, KEY_WIDTH), jnp.float32)
    rate = jnp.exp(math.log(2.5e-06) + level * math.log(3e-05 / 2.5e-06))
    shift_floor_amount = -jnp.repeat(rate, TOK_DEV, axis=0)
    spots = jax.random.randint(jax.random.fold_in(key, 32), (3,), 0, SEQ)
    leftover_stick = jax.random.uniform(jax.random.fold_in(key, 33), (3, KEY_WIDTH), jnp.float32, 0.2, 0.5)
    stick_fraction = (jnp.arange(SEQ, dtype=jnp.int32)[:, None] == spots[None, :]).astype(jnp.float32)
    segment_tile = jnp.dot(stick_fraction, jnp.log(1.0 - leftover_stick), precision=jax.lax.Precision.HIGHEST)
    return (shift_floor_amount + segment_tile).astype(jnp.float32)


def block_levels(key, extent, cuts, smallest, top_value):
    factor_of, own = 1.0, jax.random.fold_in(key, 6)
    for dim, parts in cuts:
        heights = jnp.exp(jax.random.uniform(jax.random.fold_in(own, dim), (parts,), jnp.float32, smallest / len(cuts), top_value / len(cuts)))
        factor_of = factor_of * jnp.repeat(heights, extent[dim] // parts).reshape([-1 if axis == dim else 1 for axis in range(len(extent))])
    return factor_of


def noise(stream_key, dims, spread, bound, cuts=(), kind=jnp.bfloat16):
    drawn = jax.random.normal(stream_key, dims, jnp.float32) * spread
    if len(cuts) > 0:
        drawn = block_levels(stream_key, dims, cuts, -0.22, 0.18) * drawn
    return jnp.clip(drawn, min=-bound, max=bound).astype(kind)


def setup_inputs(seed: int = 0, part: int = 0) -> dict:
    key_of = jax.random.split(jax.random.key(seed), 15)
    own_keys = jax.random.split(jax.random.fold_in(key_of[14], part), 15)
    return {
        "tokens": noise(own_keys[0], (SEQ, D), 1.0, 6.0, ((0, 64), (1, 4))),
        "norm_gain": jnp.clip(1.0 + 0.18 * jax.random.normal(key_of[1], (D,), jnp.float32), 0.1, 1.9),
        "att_q_weight": noise(key_of[2], (ATT_WIDTH, D), (2 * D ** -0.5), 0.625, ((0, 4), (1, 64))),
        "att_k_weight": noise(key_of[3], (KV_WIDTH, D), D ** -0.5, 0.125, ((0, 4), (1, 64))),
        "att_v_weight": noise(key_of[4], (KV_WIDTH, D), D ** -0.5, 0.125, ((0, 4), (1, 64))),
        "rec_q_weight": noise(key_of[5], (KEY_WIDTH, D), D ** -0.5, 0.125, ((0, 4), (1, 64))),
        "rec_f_weight": noise(key_of[6], (KEY_WIDTH, D), D ** -0.5, 0.125, ((0, 4), (1, 64))),
        "rec_i_weight": noise(key_of[7], (VAL_WIDTH, D), D ** -0.5, 0.125, ((0, 4), (1, 64))),
        "att_out_weight": noise(key_of[8], (ATT_WIDTH, D), (3 * ATT_WIDTH ** -0.5), 1.5, ((0, 4), (1, 64))),
        "rec_out_weight": noise(key_of[9], (VAL_WIDTH, D), VAL_WIDTH ** -0.5, 0.1875, ((0, 4), (1, 64))),
        "score_offset": draw_score_offset(jax.random.fold_in(key_of[14], 71), part),
        "lower_bound": draw_lower_bound(jax.random.fold_in(key_of[14], 71), part),
        "decay_shift": draw_decay_shift(jax.random.fold_in(jax.random.fold_in(key_of[14], part), 71), part),
        "rec_gain": jnp.clip(1.0 + 0.18 * jax.random.normal(key_of[13], (VAL_WIDTH,), jnp.float32), 0.1, 1.9),
    }


EPS = 1e-06
TOP_PRECISION = lax.Precision.HIGHEST

def rounded(values):
    return lax.optimization_barrier(values.astype(jnp.bfloat16))

def block_pass(carry, inputs):
    state_matrix = carry
    query_rows, log_decay, keyed_values, value_rows = inputs
    span = query_rows.shape[0]
    cumulative_log = jnp.cumsum(log_decay, axis=0)
    lower = jnp.arange(span, dtype=jnp.int32)[:, None] >= jnp.arange(span, dtype=jnp.int32)[None, :]
    diff = cumulative_log[:, None] - cumulative_log[None, :]
    decay = jnp.exp(jnp.where(lower[:, :, None, None], diff, -jnp.inf))
    score = jnp.einsum('thk,tshk,shk->ths', query_rows, decay, keyed_values, precision=TOP_PRECISION)
    inner = jnp.einsum('ths,shv->thv', score, value_rows, precision=TOP_PRECISION)
    outer_product = jnp.einsum('ril,ilc->ric', query_rows * jnp.exp(cumulative_log), state_matrix, precision=TOP_PRECISION)
    final_state = cumulative_log[-1]
    state_matrix = state_matrix * jnp.exp(final_state)[:, :, None] + jnp.einsum('iag,iax->agx', keyed_values * jnp.exp(final_state[None] - cumulative_log), value_rows, precision=TOP_PRECISION)
    return (state_matrix, inner + outer_product)

def reference(tokens, norm_gain, att_q_weight, att_k_weight, att_v_weight, rec_q_weight, rec_f_weight, rec_i_weight, att_out_weight, rec_out_weight, score_offset, lower_bound, decay_shift, rec_gain):
    raw = tokens.astype(jnp.float32)
    scaled = (raw * norm_gain[None, :]).astype(jnp.bfloat16)
    inv_rms = lax.rsqrt(lax.optimization_barrier(jnp.mean(raw * raw, axis=1)) + EPS)

    def project(weight):
        return rounded(jnp.dot(scaled, weight.T, preferred_element_type=jnp.float32) * inv_rms[:, None])
    att_query = project(att_q_weight)
    att_key = project(att_k_weight)
    att_value = project(att_v_weight)
    rec_query = project(rec_q_weight)
    rec_forget = project(rec_f_weight)
    rec_input = project(rec_i_weight)
    group = ATT_HEADS // KV_HEADS
    qblock = min(128, SEQ)
    queries = att_query.astype(jnp.float32).reshape(SEQ // qblock, qblock, KV_HEADS, group, HEAD)
    keys = att_key.astype(jnp.float32).reshape(SEQ, KV_HEADS, HEAD)
    values = att_value.astype(jnp.float32).reshape(SEQ, KV_HEADS, HEAD)
    offsets = score_offset.reshape(KV_HEADS, group)
    starts = jnp.arange(SEQ // qblock, dtype=jnp.int32) * qblock
    key_pos = jnp.arange(SEQ, dtype=jnp.int32)

    def attend(args):
        query_block, first = args
        score = jnp.einsum('tkgd,skd->tkgs', query_block, keys, precision=TOP_PRECISION) * HEAD ** (-0.5) + offsets[None, :, :, None]
        query_pos = first + jnp.arange(qblock, dtype=jnp.int32)
        visible = (key_pos[None, :] < query_pos[:, None])[:, None, None, :]
        keep = jnp.where(visible, jax.nn.log_sigmoid(-score), 0.0)
        tail = lax.cumsum(keep, axis=3, reverse=True) - keep
        weight = jnp.where(visible, jnp.exp(jax.nn.log_sigmoid(score) + tail), 0.0)
        weight = rounded(weight).astype(jnp.float32)
        return jnp.einsum('tkgs,skd->tkgd', weight, values, precision=TOP_PRECISION)
    att_out = lax.map(attend, (queries, starts)).reshape(SEQ, ATT_WIDTH).astype(jnp.bfloat16)
    logit = rec_forget.astype(jnp.float32)
    gap = 1.0 - lower_bound
    log_decay = jnp.log(lower_bound + gap * jax.nn.sigmoid(logit)) + decay_shift
    keyed_values = gap * jax.nn.sigmoid(-logit)
    rec_q = jax.nn.silu(rec_query.astype(jnp.float32))
    blocks = SEQ // SPAN

    def split(array, depth):
        return array.reshape(blocks, SPAN, RECURRENT_COUNT, depth)
    start_state = jnp.zeros((RECURRENT_COUNT, REC_KEY, REC_VAL), jnp.float32)
    _, rec_raw = lax.scan(block_pass, start_state, (split(rec_q, REC_KEY), split(log_decay, REC_KEY), split(keyed_values, REC_KEY), split(rec_input.astype(jnp.float32), REC_VAL)))
    rec_raw = rec_raw.reshape(SEQ, RECURRENT_COUNT, REC_VAL)
    rescaled_input = rec_raw * lax.rsqrt(lax.optimization_barrier(jnp.mean(rec_raw * rec_raw, axis=2, keepdims=True)) + EPS) * rec_gain.reshape(RECURRENT_COUNT, REC_VAL)
    rec_out = rescaled_input.reshape(SEQ, VAL_WIDTH).astype(jnp.bfloat16)
    att_cols = ATT_WIDTH // N_TP
    rec_cols = VAL_WIDTH // N_TP
    total = jnp.zeros((SEQ, D), jnp.float32)
    for group_index in range(N_TP):
        att_part = att_out[:, group_index * att_cols:(group_index + 1) * att_cols]
        rec_part = rec_out[:, group_index * rec_cols:(group_index + 1) * rec_cols]
        partial_value = jnp.dot(att_part, att_out_weight[group_index * att_cols:(group_index + 1) * att_cols], preferred_element_type=jnp.float32)
        partial_value = partial_value + jnp.dot(rec_part, rec_out_weight[group_index * rec_cols:(group_index + 1) * rec_cols], preferred_element_type=jnp.float32)
        total = total + rounded(partial_value).astype(jnp.float32)
    return total.astype(jnp.bfloat16)
```

```python
import functools

import jax
import jax.numpy as jnp
from jax import lax
from jax.experimental import pallas as pl
from jax.experimental.pallas import tpu as pltpu
from jax.sharding import PartitionSpec as P

HEAD = 64
REC = 128
EPS = 1e-06
LOG2E = 1.4426950408889634
MESH = pl.DeviceIdType.MESH
F32 = jnp.float32
BF16 = jnp.bfloat16

PARTS = 4
KV_PARTS = 5
DECAY_ROWS = 16


def nt(a, b):
    return lax.dot_general(a, b, (((1,), (1,)), ((), ())), preferred_element_type=F32)


def nn(a, b):
    return lax.dot_general(a, b, (((1,), (0,)), ((), ())), preferred_element_type=F32)


def iota(shape, dim):
    return lax.broadcasted_iota(jnp.int32, shape, dim)


def greet(devices):
    barrier = pltpu.get_barrier_semaphore()
    for device in devices:
        pl.semaphore_signal(barrier, inc=1, device_id=device, device_id_type=MESH)
    pl.semaphore_wait(barrier, len(devices))


def place(nz):
    sp = lax.axis_index("sp")
    z, c = sp // 2, sp % 2
    partner = {"sp": 2 * z + 1 - c}
    up = {"sp": 2 * ((z + 1) % nz) + c}
    down = {"sp": 2 * ((z + nz - 1) % nz) + c}
    return z, c, partner, up, down


def send(src, dst, send_sem, recv_sem, device):
    return pltpu.make_async_remote_copy(
        src_ref=src,
        dst_ref=dst,
        send_sem=send_sem,
        recv_sem=recv_sem,
        device_id=device,
        device_id_type=MESH,
    )


def gather_kernel(
    nz, ntp, tok, wt, shift, xg, w, shift_out,
    ring_send, ring_recv, swap_send, swap_recv, tok_send, tok_recv,
    relay_send, relay_recv, shift_send, shift_recv, local_sem,
):
    z, c, partner, up, down = place(nz)
    x = lax.axis_index("tp")
    ways = ((up, 0, nz // 2, -1), (down, 1, nz - 1 - nz // 2, 1))
    half = PARTS // 2
    greet([partner, up, down] + [{"tp": (x + i) % ntp} for i in range(1, ntp)])

    locals_, swaps, toks, relays = [], [], [], []
    for p in range(half):
        swaps.append(
            send(wt.at[1 - c, p], w.at[z, half * c + p], swap_send.at[p], swap_recv.at[p], partner)
        )
        locals_.append(
            pltpu.make_async_copy(wt.at[c, p], w.at[z, half * c + p], local_sem.at[p])
        )
    for swap in swaps:
        swap.start()
    first = []
    for p in range(half):
        j = half * c + p
        for device, way, count, _ in ways:
            if count > 0:
                first.append(
                    send(wt.at[c, p], w.at[z, j], ring_send.at[way, 0, j], ring_recv.at[way, 0, j], device)
                )
                first[-1].start()
    for i in range(1, ntp):
        toks.append(
            send(tok, xg.at[x, c], tok_send.at[i - 1], tok_recv.at[i - 1], {"tp": (x + i) % ntp})
        )
        toks[-1].start()
    for p in range(half):
        j = half * (1 - c) + p
        swaps[p].wait_recv()
        for device, way, count, _ in ways:
            if count > 0:
                first.append(
                    send(w.at[z, j], w.at[z, j], ring_send.at[way, 0, j], ring_recv.at[way, 0, j], device)
                )
                first[-1].start()
    relays.append(send(tok, xg.at[x, c], relay_send.at[0], relay_recv.at[0], partner))
    relays[-1].start()
    own = pl.ds(pl.multiple_of(REC * c, REC), REC)
    other = pl.ds(pl.multiple_of(REC * (1 - c), REC), REC)
    shift_copy = send(shift.at[:, other], shift_out.at[c], shift_send, shift_recv, partner)
    shift_copy.start()
    locals_.append(pltpu.make_async_copy(tok, xg.at[x, c], local_sem.at[half]))
    locals_.append(pltpu.make_async_copy(shift.at[:, own], shift_out.at[c], local_sem.at[half + 1]))
    for copy in locals_:
        copy.start()

    def hop(way, d, j, device, sign):
        slot = (z + sign * (d - 1) + nz) % nz
        ref = w.at[slot, j]
        return send(ref, ref, ring_send.at[way, d - 1, j], ring_recv.at[way, d - 1, j], device)

    def arrived(way, d, j, device, sign):
        ref = w.at[(z + sign * d + nz) % nz, j]
        send(ref, ref, ring_send.at[way, d - 1, j], ring_recv.at[way, d - 1, j], device).wait_recv()

    def forward(d, some):
        for j in range(PARTS):
            for device, way, _, sign in some:
                arrived(way, d - 1, j, device, sign)
                hop(way, d, j, device, sign).start()

    def body(d, _):
        forward(d, ways)
        return 0

    both = min(count for _, _, count, _ in ways)
    middle = max(min(both + 1, 6), 2)
    lax.fori_loop(2, middle, body, 0)
    for i in range(1, ntp):
        toks[i - 1].wait_recv()
        ref = xg.at[(x + ntp - i) % ntp, c]
        relays.append(send(ref, ref, relay_send.at[i], relay_recv.at[i], partner))
        relays[-1].start()
    lax.fori_loop(middle, both + 1, body, 0)
    for d in range(both + 1, ways[0][2] + 1):
        if d > 1:
            forward(d, ways[:1])
    for device, way, count, sign in ways:
        for j in range(PARTS):
            if count > 0:
                arrived(way, count, j, device, sign)

    def drain(d, _):
        for j in range(PARTS):
            for device, way, _, sign in ways:
                hop(way, d, j, device, sign).wait_send()
        return 0

    for copy in first:
        copy.wait_send()
    lax.fori_loop(2, both + 1, drain, 0)
    for d in range(max(both + 1, 2), ways[0][2] + 1):
        for j in range(PARTS):
            hop(0, d, j, up, -1).wait_send()
    for copy in swaps + toks:
        copy.wait_send()
    for copy in relays:
        copy.wait()
    shift_copy.wait()
    for copy in locals_:
        copy.wait()


def gather(nz, ntp, tokens, wt, shift):
    rows, width = tokens.shape
    cols = wt.shape[-1]
    steps = nz // 2
    dma = pltpu.SemaphoreType.DMA
    vmem = pl.BlockSpec(memory_space=pltpu.VMEM)
    return pl.pallas_call(
        functools.partial(gather_kernel, nz, ntp),
        out_shape=(
            jax.ShapeDtypeStruct((ntp, 2, rows, width), BF16),
            jax.ShapeDtypeStruct((nz, PARTS, wt.shape[2], cols), BF16),
            jax.ShapeDtypeStruct((2, rows, REC), F32),
        ),
        in_specs=[vmem] * 3,
        out_specs=(vmem,) * 3,
        scratch_shapes=[
            dma((2, steps, PARTS)), dma((2, steps, PARTS)),
            dma((PARTS // 2,)), dma((PARTS // 2,)),
            dma((ntp - 1,)), dma((ntp - 1,)),
            dma((ntp,)), dma((ntp,)),
            dma, dma, dma((PARTS // 2 + 2,)),
        ],
        compiler_params=pltpu.CompilerParams(collective_id=0, has_side_effects=True),
        name="gather_weights",
    )(tokens, wt, shift)


def split3(a):
    hi = a.astype(BF16)
    rest = a - hi.astype(F32)
    mid = rest.astype(BF16)
    low = (rest - mid.astype(F32)).astype(BF16)
    return hi, mid, low


def project_kernel(
    ntp, xg, gain, w, lower, shift, q2, chunk, reach, inner, wv, sem
):
    rows = 2 * xg.shape[2]
    width = xg.shape[3]
    skip = 2 * REC
    copy = pltpu.make_async_copy(w.at[:, :, :, skip:], wv, sem)
    copy.start()
    sq = jnp.zeros((rows, 1), F32)
    scaled = []
    for i in range(ntp):
        raw = xg[i].reshape(rows, width).astype(F32)
        sq = sq + jnp.sum(raw * raw, axis=1, keepdims=True)
        scaled.append((raw * gain[:, i * width : (i + 1) * width]).astype(BF16))
    inv = lax.rsqrt(sq / (ntp * width) + EPS)
    copy.wait()
    per = wv.shape[0] // ntp
    total = None
    for i in range(ntp):
        part = nn(scaled[i], wv[i * per : (i + 1) * per].reshape(width, wv.shape[3]))
        total = part if total is None else total + part
    total = (total * inv).astype(BF16)
    lane = iota((rows, REC), 1)
    q = total[:, :REC].astype(F32)
    q2[0:rows] = jnp.where(lane < HEAD, q, 0.0).astype(BF16)
    q2[rows : 2 * rows] = jnp.where(lane < HEAD, pltpu.roll(q, HEAD, 1), 0.0).astype(BF16)
    chunk[0:rows] = total[:, REC : 2 * REC]
    rq = total[:, 2 * REC : 3 * REC].astype(F32)
    logit = total[:, 3 * REC : 4 * REC].astype(F32)
    vi = total[:, 4 * REC : 5 * REC]
    rq = rq / (1.0 + jnp.exp(-rq))
    low = lower[...]
    gap = 1.0 - low
    e = jnp.exp(-jnp.abs(logit))
    small, large = e / (1.0 + e), 1.0 / (1.0 + e)
    up = logit >= 0.0
    sig, neg = jnp.where(up, large, small), jnp.where(up, small, large)
    log_decay = jnp.log(low + gap * sig) + shift[...].reshape(rows, REC)
    key = gap * neg

    t, j = iota((rows, rows), 0), iota((rows, rows), 1)
    pieces = jnp.concatenate(split3(log_decay), axis=1)

    def summed(mask):
        s = nn(mask.astype(F32).astype(BF16), pieces)
        return s[:, :REC] + s[:, REC : 2 * REC] + s[:, 2 * REC :]

    cum = summed(j <= t)
    reach[...] = (rq * jnp.exp(cum)).astype(BF16)
    late = (key * jnp.exp(summed(j > t))).astype(BF16)
    state = lax.dot_general(vi, late, (((0,), (0,)), ((), ())), preferred_element_type=F32)
    chunk[rows : rows + REC] = state.astype(BF16)
    hi, mid, low3 = split3(cum[rows - 1 : rows, :])
    row = iota((DECAY_ROWS, REC), 0)
    decay = jnp.where(
        row == 0, hi.astype(F32), jnp.where(row == 1, mid.astype(F32), jnp.where(row == 2, low3.astype(F32), 0.0))
    )
    chunk[rows + REC :] = decay.astype(BF16)

    score = jnp.where(t == j, jnp.sum(rq * key, axis=1, keepdims=True), 0.0)
    h = 1
    while h < rows:
        base = t - (t & (2 * h - 1))
        mid_t = base + (h - 1)
        factor = jnp.exp(summed((j > jnp.minimum(t, mid_t)) & (j <= jnp.maximum(t, mid_t))))
        level = nt((rq * factor).astype(BF16), (key * factor).astype(BF16))
        score = jnp.where((t > mid_t) & (j >= base) & (j <= mid_t), level, score)
        h *= 2
    inner[...] = nn(score.astype(BF16), vi)


def project(ntp, xg, gain, w, lower, shift):
    rows = 2 * xg.shape[2]
    vmem = pl.BlockSpec(memory_space=pltpu.VMEM)
    return pl.pallas_call(
        functools.partial(project_kernel, ntp),
        out_shape=(
            jax.ShapeDtypeStruct((2 * rows, REC), BF16),
            jax.ShapeDtypeStruct((rows + REC + DECAY_ROWS, REC), BF16),
            jax.ShapeDtypeStruct((rows, REC), BF16),
            jax.ShapeDtypeStruct((rows, REC), F32),
        ),
        in_specs=[vmem, vmem, pl.BlockSpec(memory_space=pl.ANY), vmem, vmem],
        out_specs=(vmem,) * 4,
        scratch_shapes=[
            pltpu.VMEM((*w.shape[:3], w.shape[3] - 2 * REC), BF16),
            pltpu.SemaphoreType.DMA,
        ],
        name="project",
    )(xg, gain, w, lower, shift)


def mix_kernel(
    nz, chunk, q2, offset, reach, inner, gain, att, rec,
    buf, later, near, run, far, state_near, state_run, state_far, ring_send, ring_recv,
):
    z, _, _, up, down = place(nz)
    ways = ((up, 0, nz // 2, -1), (down, 1, nz - 1 - nz // 2, 1))
    rows = q2.shape[0] // 2
    heads = 2
    greet([up, down])

    def slot_of(d, sign):
        return (z + sign * d + nz) % nz

    def hop(way, d, j, device, sign):
        ref = buf.at[slot_of(d - 1, sign), j]
        return send(ref, ref, ring_send.at[way, d - 1, j], ring_recv.at[way, d - 1, j], device)

    def arrived(way, d, j, device, sign):
        ref = buf.at[slot_of(d, sign), j]
        send(ref, ref, ring_send.at[way, d - 1, j], ring_recv.at[way, d - 1, j], device).wait_recv()

    first = []
    for j in range(KV_PARTS):
        for device, way, count, _ in ways:
            if count > 0:
                first.append(
                    send(chunk.at[j], buf.at[z, j], ring_send.at[way, 0, j], ring_recv.at[way, 0, j], device)
                )
                first[-1].start()

    t, j = iota((rows, rows), 0), iota((rows, rows), 1)
    later[...] = (t > j).astype(F32).astype(BF16)
    state_near[...] = jnp.zeros_like(state_near)
    state_far[...] = jnp.zeros_like(state_far)
    state_run[...] = jnp.zeros_like(state_run)
    far[...] = jnp.zeros_like(far)

    def scores(h, kv, mask=None):
        s2 = nt(q2[h * rows : (h + 1) * rows], kv) * (HEAD**-0.5 * LOG2E) + offset[h] * LOG2E
        soft = jnp.log(1.0 + jnp.exp2(-jnp.abs(s2))) * LOG2E
        spent = jnp.maximum(s2, 0.0) + soft
        gain2 = jnp.minimum(s2, 0.0) - soft
        if mask is not None:
            spent = jnp.where(mask, spent, 0.0)
        hi = spent.astype(BF16)
        lo = (spent - hi.astype(F32)).astype(BF16)
        tail = nn(hi, later[...]) + nn(lo, later[...])
        return gain2 - tail, tail[:, 0:1] + spent[:, 0:1]

    flat = chunk[...].reshape(-1, REC)
    kv = flat[:rows]
    seen = j < t
    for h in range(heads):
        own = slice(h * rows, (h + 1) * rows)
        power, total = scores(h, kv, seen)
        weight = jnp.where(seen, jnp.exp2(power), 0.0).astype(BF16)
        near[own] = nn(weight, kv)
        run[own] = total

    def decay_of(block):
        rows3 = block[rows + REC : rows + REC + 8].astype(F32)
        return rows3[0:1] + rows3[1:2] + rows3[2:3]

    def use_near(d):
        @pl.when(z - d >= 0)
        def _():
            block = buf[slot_of(d, -1)].reshape(-1, REC)
            kv = block[:rows]
            for h in range(heads):
                own = slice(h * rows, (h + 1) * rows)
                power, total = scores(h, kv)
                before = run[own]
                near[own] += nn(jnp.exp2(power - before).astype(BF16), kv)
                run[own] = before + total
            before = state_run[...]
            state_near[...] += jnp.exp(before) * block[rows : rows + REC].astype(F32)
            state_run[...] = before + decay_of(block)

    def use_far(d):
        @pl.when(z + d >= nz)
        def _():
            block = buf[slot_of(d, 1)].reshape(-1, REC)
            kv = block[:rows]
            for h in range(heads):
                own = slice(h * rows, (h + 1) * rows)
                power, total = scores(h, kv)
                far[own] = far[own] * jnp.exp2(-total) + nn(jnp.exp2(power).astype(BF16), kv)
            state_far[...] = state_far[...] * jnp.exp(decay_of(block)) + block[rows : rows + REC].astype(F32)

    def forward(d, some):
        for j in range(KV_PARTS):
            for device, way, _, sign in some:
                arrived(way, d - 1, j, device, sign)
                hop(way, d, j, device, sign).start()

    def body(d, _):
        forward(d, ways)
        use_near(d - 1)
        use_far(d - 1)
        return 0

    both = min(count for _, _, count, _ in ways)
    most = ways[0][2]
    lax.fori_loop(2, both + 1, body, 0)
    for d in range(max(both + 1, 2), most + 1):
        forward(d, ways[:1])
        if d == both + 1:
            for j in range(KV_PARTS):
                arrived(1, both, j, down, 1)
            use_near(both)
            use_far(both)
        else:
            use_near(d - 1)
    for j in range(KV_PARTS):
        arrived(0, most, j, up, -1)
    use_near(most)

    lane = iota((rows, REC), 1)
    outs = []
    for h in range(heads):
        own = slice(h * rows, (h + 1) * rows)
        outs.append(near[own] + jnp.exp2(-run[own]) * far[own])
    att[...] = jnp.where(lane < HEAD, pltpu.roll(outs[0], HEAD, 1), outs[1]).astype(BF16)
    state = state_near[...] + jnp.exp(state_run[...]) * state_far[...]
    raw = inner[...] + nt(reach[...], state.astype(BF16))
    mean = jnp.sum(raw * raw, axis=1, keepdims=True) / REC
    rec[...] = (raw * lax.rsqrt(mean + EPS) * gain[...]).astype(BF16)

    for copy in first:
        copy.wait_send()

    def drain(d, _):
        for j in range(KV_PARTS):
            for device, way, _, sign in ways:
                hop(way, d, j, device, sign).wait_send()
        return 0

    lax.fori_loop(2, both + 1, drain, 0)
    for d in range(max(both + 1, 2), most + 1):
        for j in range(KV_PARTS):
            hop(0, d, j, up, -1).wait_send()


def mix(nz, chunk, q2, offset, reach, inner, gain):
    rows = reach.shape[0]
    steps = nz // 2
    dma = pltpu.SemaphoreType.DMA
    vmem = pl.BlockSpec(memory_space=pltpu.VMEM)
    chunk = chunk.reshape(KV_PARTS, -1, REC)
    return pl.pallas_call(
        functools.partial(mix_kernel, nz),
        out_shape=(
            jax.ShapeDtypeStruct((rows, REC), BF16),
            jax.ShapeDtypeStruct((rows, REC), BF16),
        ),
        in_specs=[vmem, vmem, pl.BlockSpec(memory_space=pltpu.SMEM), vmem, vmem, vmem],
        out_specs=(vmem,) * 2,
        scratch_shapes=[
            pltpu.VMEM((nz, *chunk.shape), BF16),
            pltpu.VMEM((rows, rows), BF16),
            pltpu.VMEM((2 * rows, REC), F32),
            pltpu.VMEM((2 * rows, 1), F32),
            pltpu.VMEM((2 * rows, REC), F32),
            pltpu.VMEM((REC, REC), F32),
            pltpu.VMEM((1, REC), F32),
            pltpu.VMEM((REC, REC), F32),
            dma((2, steps, KV_PARTS)), dma((2, steps, KV_PARTS)),
        ],
        compiler_params=pltpu.CompilerParams(collective_id=1, has_side_effects=True),
        name="mix",
    )(chunk, q2, offset, reach, inner, gain)


def out_kernel(
    nz, ntp, att, rec, w, out, wv, away, back, home, parts, got,
    w_sem, swap_send, swap_recv, part_send, part_recv,
):
    _, c, partner, _, _ = place(nz)
    x = lax.axis_index("tp")
    half = att.shape[0] // 2
    share = half // ntp
    copy = pltpu.make_async_copy(w.at[:, :, :, : 2 * REC], wv, w_sem)
    copy.start()
    greet([partner] + [{"tp": (x + i) % ntp} for i in range(1, ntp)])
    copy.wait()
    weights = wv[...].reshape(-1, 2 * REC)

    def partial(core):
        own = pl.ds(pl.multiple_of(half * core, half), half)
        return nt(jnp.concatenate([att[own, :], rec[own, :]], axis=1), weights)

    away[...] = partial(1 - c).astype(BF16)
    swap = send(away, back, swap_send, swap_recv, partner)
    swap.start()
    home[...] = partial(c)
    swap.wait_recv()
    total = home[...] + back[...].astype(F32)
    parts[...] = total.astype(BF16).reshape(ntp, share, -1)
    copies = []
    for i in range(1, ntp):
        copies.append(
            send(parts.at[(x + i) % ntp], got.at[i - 1], part_send.at[i - 1], part_recv.at[i - 1], {"tp": (x + i) % ntp})
        )
        copies[-1].start()
    result = parts[x].astype(F32)
    for i in range(1, ntp):
        copies[i - 1].wait_recv()
        result = result + got[i - 1].astype(F32)
    out[...] = result.astype(BF16)
    swap.wait_send()
    for copy in copies:
        copy.wait_send()


def project_out(nz, ntp, att, rec, w):
    rows = att.shape[0]
    half = rows // 2
    width = w.shape[0] * w.shape[1] * w.shape[2]
    dma = pltpu.SemaphoreType.DMA
    vmem = pl.BlockSpec(memory_space=pltpu.VMEM)
    return pl.pallas_call(
        functools.partial(out_kernel, nz, ntp),
        out_shape=jax.ShapeDtypeStruct((half // ntp, width), BF16),
        in_specs=[vmem, vmem, pl.BlockSpec(memory_space=pl.ANY)],
        out_specs=vmem,
        scratch_shapes=[
            pltpu.VMEM((*w.shape[:3], 2 * REC), BF16),
            pltpu.VMEM((half, width), BF16),
            pltpu.VMEM((half, width), BF16),
            pltpu.VMEM((half, width), F32),
            pltpu.VMEM((ntp, half // ntp, width), BF16),
            pltpu.VMEM((ntp - 1, half // ntp, width), BF16),
            dma, dma, dma, dma((ntp - 1,)), dma((ntp - 1,)),
        ],
        compiler_params=pltpu.CompilerParams(collective_id=2, has_side_effects=True),
        name="project_out",
    )(att, rec, w)


def on_device(
    nz,
    ntp,
    tokens,
    norm_gain,
    att_q_weight,
    att_k_weight,
    att_v_weight,
    rec_q_weight,
    rec_f_weight,
    rec_i_weight,
    att_out_weight,
    rec_out_weight,
    score_offset,
    lower_bound,
    decay_shift,
    rec_gain,
):
    c = lax.axis_index("sp") % 2

    def halves(weight):
        return weight.reshape(2, weight.shape[0] // 2, weight.shape[1])

    wt = jnp.concatenate(
        [
            halves(weight)
            for weight in (
                att_out_weight,
                rec_out_weight,
                att_q_weight,
                att_k_weight,
                att_v_weight,
                rec_q_weight,
                rec_f_weight,
                rec_i_weight,
            )
        ],
        axis=1,
    ).transpose(0, 2, 1)
    wt = wt.reshape(2, PARTS // 2, -1, wt.shape[2])
    xg, w, shift = gather(nz, ntp, tokens, wt, decay_shift)
    lower = lax.dynamic_index_in_dim(lower_bound.reshape(2, 1, REC), c, 0, keepdims=False)
    gain = lax.dynamic_index_in_dim(rec_gain.reshape(2, 1, REC), c, 0, keepdims=False)
    offset = lax.dynamic_index_in_dim(score_offset.reshape(2, 2), c, 0, keepdims=False)
    q2, chunk, reach, inner = project(ntp, xg, norm_gain.reshape(1, -1), w, lower, shift)
    att, rec = mix(nz, chunk, q2, offset, reach, inner, gain)
    return project_out(nz, ntp, att, rec, w)


def solution(mesh):
    in_specs = (
        P(("grp", "sp"), "tp"),
        P(),
        P("tp", "sp"),
        P("tp", "sp"),
        P("tp", "sp"),
        P("tp", "sp"),
        P("tp", "sp"),
        P("tp", "sp"),
        P("tp", "sp"),
        P("tp", "sp"),
        P("tp"),
        P("tp"),
        P(("grp", "sp"), "tp"),
        P("tp"),
    )
    out_specs = P(("grp", "sp", "tp"), None)
    return jax.shard_map(
        functools.partial(on_device, mesh.shape["sp"] // 2, mesh.shape["tp"]),
        mesh=mesh,
        in_specs=in_specs,
        out_specs=out_specs,
        check_vma=False,
    )
```
